32 devices in a mesh: sp: 4 (over z), dp: 8 (over y, x, core).
Axes of the slice: x: 2, y: 2, z: 4, core: 2. Of those that a mesh axis runs over, the one named last changes fastest.
Arguments:
- value_half: bfloat16 [8, 1536, 2048], P('dp', 'sp'), may hold values from -6 to 6
- gate_half: bfloat16 [8, 1536, 2048], P('dp', 'sp'), may hold values from -9 to 9
- conv_taps: bfloat16 [31, 2048], replicated, may hold values from -1 to 1
- norm_gain: float32 [2048], replicated, may hold values from 0.1 to 1.9
- norm_shift: float32 [2048], replicated, may hold values from -3 to 3
- out_weight: bfloat16 [2048, 2048], P('dp', 'sp'), may hold values from -0.125 to 0.125
Outputs:
- module_out: bfloat16 [8, 1536, 2048], P('dp', 'sp')
The draws below stay inside these ranges and needn't reach their ends.
All inputs are finite; a program needn't handle non-finite values.
Results may differ from the reference program's by a relative error of at most 0.0064.
Values may be sent and summed in bfloat16 or wider, within the bound.
No kernel may reach another device: no remote copies, remote signals or barrier semaphores. Data moves between devices by JAX's collectives and lax.ppermute only.
A program may use at most 64 MiB of HBM per device.

```python
import jax
import jax.numpy as jnp
from jax import lax

D = 2048
CONV_W = 31
SEQ_LEN = 1536
SEQS = 8


def steps_of(stream_key, shape, shards, least, top_value):
    factor_of, own = 1.0, jax.random.fold_in(stream_key, 6)
    for position, shards_of in shards:
        heights = jnp.exp(jax.random.uniform(jax.random.fold_in(own, position), (shards_of,), jnp.float32, least / len(shards), top_value / len(shards)))
        factor_of = factor_of * jnp.repeat(heights, shape[position] // shards_of).reshape([-1 if axis == position else 1 for axis in range(len(shape))])
    return factor_of


def noise(own_key, shape, scale, limit, pieces=(), kind=jnp.bfloat16):
    values = jax.random.normal(own_key, shape, jnp.float32) * scale
    if len(pieces) > 0:
        values = steps_of(own_key, shape, pieces, -0.22, 0.18) * values
    return jnp.clip(values, min=-limit, max=limit).astype(kind)


def setup_inputs(seed: int = 0) -> dict:
    keys = jax.random.split(jax.random.key(seed), 7)
    value_half = noise(keys[0], (SEQS, SEQ_LEN, D), 1.0, 6.0, ((0, 8), (1, 4)))
    gate_half = noise(keys[1], (SEQS, SEQ_LEN, D), 1.5, 9.0, ((0, 8), (1, 4)))
    conv_taps = noise(keys[2], (CONV_W, D), CONV_W ** -0.5, 1.0)
    norm_gain = jnp.clip(1.0 + 0.18 * jax.random.normal(keys[3], (D,), jnp.float32), 0.1, 1.9)
    norm_shift = noise(keys[4], (D,), 0.5, 3.0, (), jnp.float32)
    out_weight = noise(keys[5], (D, D), D ** -0.5, 0.125, ((0, 8), (1, 4)))
    return {"value_half": value_half, "gate_half": gate_half, "conv_taps": conv_taps, "norm_gain": norm_gain, "norm_shift": norm_shift, "out_weight": out_weight}


EPSILON = 1e-06

def causal_mix(gated, conv_taps):
    tap_count = conv_taps.shape[0]
    length = gated.shape[0]
    padded = jnp.concatenate([jnp.zeros((tap_count - 1, gated.shape[1]), gated.dtype), gated], 0)
    running = jnp.zeros((length, gated.shape[1]), jnp.float32)
    for tap_index in range(tap_count):
        running = running + padded[tap_index:tap_index + length].astype(jnp.float32) * conv_taps[tap_index].astype(jnp.float32)
    return running.astype(jnp.bfloat16)

def one_sequence(pair, conv_taps, norm_gain, norm_shift, out_weight):
    value_rows, gate_rows = pair
    gated = (value_rows.astype(jnp.float32) * jax.nn.sigmoid(gate_rows.astype(jnp.float32))).astype(jnp.bfloat16)
    convolved = causal_mix(gated, conv_taps).astype(jnp.float32)
    mean_row = lax.optimization_barrier(jnp.mean(convolved, axis=-1, keepdims=True))
    centered = convolved - mean_row
    variance = lax.optimization_barrier(jnp.mean(centered * centered, axis=-1, keepdims=True))
    normed = centered * lax.rsqrt(variance + EPSILON) * norm_gain + norm_shift
    activated = jax.nn.silu(normed).astype(jnp.bfloat16)
    return jnp.dot(activated, out_weight, preferred_element_type=jnp.float32).astype(jnp.bfloat16)

def reference(value_half, gate_half, conv_taps, norm_gain, norm_shift, out_weight):
    return lax.map(lambda pair: one_sequence(pair, conv_taps, norm_gain, norm_shift, out_weight), (value_half, gate_half))
```

```python
import jax
import jax.numpy as jnp
from jax import lax
from jax.sharding import PartitionSpec as P

EPSILON = 1e-06


def passed_along(value, axis, steps):
    count = lax.axis_size(axis)
    initial, last = (max(0, -steps), min(count, count - steps))
    return lax.ppermute(value, axis, [(source, source + steps) for source in range(initial, last)])


def swapped(value, axis, mask_of):
    count = lax.axis_size(axis)
    return lax.ppermute(value, axis, [(index, index ^ mask_of(index)) for index in range(count)])


def bit_orders(count):
    masks = [1 << bit for bit in range(1, (count - 1).bit_length())]
    return masks, masks[::-1]


def plane_gather(piece, axis):
    forward, backward = bit_orders(lax.axis_size(axis))
    held = piece[None]
    for even, odd in zip(forward, backward):
        other = swapped(held, axis, lambda index: odd if index & 1 else even)
        held = jnp.concatenate([held, other], 0)
    partner = swapped(held, axis, lambda index: 1)
    return jnp.concatenate([held, partner], 0)


def slot_offsets(count):
    tables = []
    for parity in range(2):
        own, partner = ([0], [0])
        for step in range(len(bit_orders(count)[0])):
            own = own + [mask ^ bit_orders(count)[parity][step] for mask in own]
            partner = partner + [mask ^ bit_orders(count)[1 - parity][step] for mask in partner]
        tables.append(own + [mask ^ 1 for mask in partner])
    return tables


def causal_mix(padded, conv_taps, length):
    tap_count = conv_taps.shape[0]
    running = jnp.zeros((length, padded.shape[1]), jnp.float32)
    for tap_index in range(tap_count):
        running = running + padded[tap_index : tap_index + length].astype(jnp.float32) * conv_taps[
            tap_index
        ].astype(jnp.float32)
    return running.astype(jnp.bfloat16)


def per_device(value_half, gate_half, conv_taps, norm_gain, norm_shift, out_weight):
    tap_count = conv_taps.shape[0]
    tok_rows = value_half.shape[1]
    layers, blocks = (lax.axis_size("sp"), lax.axis_size("dp"))
    here, place = (lax.axis_index("sp"), lax.axis_index("dp"))
    gathered = []
    for step in range(layers):
        layer = out_weight if step == 0 else swapped(out_weight, "sp", lambda index: step)
        gathered.append(plane_gather(layer, "dp"))
    gated = (
        value_half[0].astype(jnp.float32) * jax.nn.sigmoid(gate_half[0].astype(jnp.float32))
    ).astype(jnp.bfloat16)
    tail_rows = gated[tok_rows - (tap_count - 1) :]
    history = passed_along(tail_rows, "sp", 1)
    padded = jnp.concatenate([history, gated], 0)
    convolved = causal_mix(padded, conv_taps, tok_rows)
    widened = convolved.astype(jnp.float32)
    mean_row = jnp.mean(widened, axis=-1, keepdims=True)
    centered = widened - mean_row
    variance = jnp.mean(centered * centered, axis=-1, keepdims=True)
    normed = centered * lax.rsqrt(variance + EPSILON) * norm_gain + norm_shift
    activated = jax.nn.silu(normed).astype(jnp.bfloat16)
    depth, width = out_weight.shape
    even, odd = slot_offsets(blocks)
    offsets = jnp.where(place % 2 == 0, jnp.array(even), jnp.array(odd))
    pieces = [
        lax.dynamic_slice_in_dim(activated, (place ^ offsets[slot]) * depth, depth, 1)
        for slot in range(blocks)
    ]
    ordered = jnp.concatenate(pieces, 1)
    out = jnp.zeros((tok_rows, layers * width), jnp.bfloat16)
    for step in range(layers):
        part = jnp.dot(
            ordered,
            gathered[step].reshape(blocks * depth, width),
            preferred_element_type=jnp.float32,
        ).astype(jnp.bfloat16)
        out = lax.dynamic_update_slice_in_dim(out, part, (here ^ step) * width, 1)
    return out[None]


def solution(mesh):
    placed = (P("dp", "sp", None), P("dp", "sp", None), P(), P(), P(), P("dp", "sp"))
    return jax.shard_map(
        per_device, mesh=mesh, in_specs=placed, out_specs=P("dp", "sp", None), check_vma=False
    )
```

```python
import functools

import jax
import jax.numpy as jnp
from jax import lax
from jax.experimental import pallas as pl
from jax.experimental.pallas import tpu as pltpu
from jax.sharding import PartitionSpec as P


EPSILON = 1e-06
LANES = 128


def swapped(value, axis, mask_of):
    count = lax.axis_size(axis)
    return lax.ppermute(value, axis, [(index, index ^ mask_of(index)) for index in range(count)])


def named(value, axis, even, odd):
    return swapped(value, axis, lambda index: odd if index & 1 else even)


def passed_along(value, axis, steps):
    count = lax.axis_size(axis)
    initial, last = (max(0, -steps), min(count, count - steps))
    return lax.ppermute(value, axis, [(source, source + steps) for source in range(initial, last)])


def plane_gather(piece, axis):
    count = lax.axis_size(axis)
    masks = [1 << bit for bit in range(1, (count - 1).bit_length())]
    held = piece[None]
    for even, odd in zip(masks, masks[::-1]):
        other = swapped(held, axis, lambda index: odd if index & 1 else even)
        held = jnp.concatenate([held, other], 0)
    return jnp.concatenate([held, swapped(held, axis, lambda index: 1)], 0)


def slot_offsets(count):
    masks = [1 << bit for bit in range(1, (count - 1).bit_length())]
    halves = []
    for order in (masks, masks[::-1]):
        held = [0]
        for mask in order:
            held = held + [offset ^ mask for offset in held]
        halves.append(held)
    return [halves[parity] + [offset ^ 1 for offset in halves[1 - parity]] for parity in range(2)]


def general(value_half, gate_half, conv_taps, norm_gain, norm_shift, out_weight):
    tap_count, tok_rows = (conv_taps.shape[0], value_half.shape[1])
    layers, blocks = (lax.axis_size("sp"), lax.axis_size("dp"))
    here, place = (lax.axis_index("sp"), lax.axis_index("dp"))
    depth, width = out_weight.shape
    gathered = [
        plane_gather(swapped(out_weight, "sp", lambda index: step) if step else out_weight, "dp")
        for step in range(layers)
    ]
    gated = (
        value_half[0].astype(jnp.float32) * jax.nn.sigmoid(gate_half[0].astype(jnp.float32))
    ).astype(jnp.bfloat16)
    history = passed_along(gated[tok_rows - (tap_count - 1) :], "sp", 1)
    padded = jnp.concatenate([history, gated], 0)
    running = jnp.zeros(gated.shape, jnp.float32)
    for tap_index in range(tap_count):
        running = running + padded[tap_index : tap_index + tok_rows].astype(jnp.float32) * conv_taps[
            tap_index
        ].astype(jnp.float32)
    widened = running.astype(jnp.bfloat16).astype(jnp.float32)
    centered = widened - jnp.mean(widened, axis=-1, keepdims=True)
    variance = jnp.mean(centered * centered, axis=-1, keepdims=True)
    normed = centered * lax.rsqrt(variance + EPSILON) * norm_gain + norm_shift
    activated = jax.nn.silu(normed).astype(jnp.bfloat16)
    even, odd = slot_offsets(blocks)
    offsets = jnp.where(place % 2 == 0, jnp.array(even), jnp.array(odd))
    ordered = jnp.concatenate(
        [
            lax.dynamic_slice_in_dim(activated, (place ^ offsets[slot]) * depth, depth, 1)
            for slot in range(blocks)
        ],
        1,
    )
    out = jnp.zeros((tok_rows, layers * width), jnp.bfloat16)
    for step in range(layers):
        part = jnp.dot(
            ordered,
            gathered[step].reshape(blocks * depth, width),
            preferred_element_type=jnp.float32,
        ).astype(jnp.bfloat16)
        out = lax.dynamic_update_slice_in_dim(out, part, (here ^ step) * width, 1)
    return out[None]


GATHERED = ((0, 2, 4, 6), (0, 4, 2, 6))
SWAPS = (((0, 1, 2, 3),), ((0, 1, 2, 3),), ((0, 1, 2, 3),), ((0, 1, 2), (3,)))


def logistic_times(value, argument):
    return value / (1.0 + jnp.exp(-argument))


def tail_kernel(value_ref, gate_ref, out_ref):
    rows = out_ref.shape[0]
    span = pl.ds(value_ref.shape[1] - rows, rows)
    value = value_ref[0, span].astype(jnp.float32)
    gate = gate_ref[0, span].astype(jnp.float32)
    out_ref[...] = logistic_times(value, gate).astype(jnp.bfloat16)


def stack_kernel(*refs):
    for index, ref in enumerate(refs[:-1]):
        refs[-1][index] = ref[...]


def mix_kernel(first_row, rows, pad, tap_count, depth, *refs):
    (value_ref, gate_ref, taps_ref, gain_ref, shift_ref) = refs[:5]
    history_ref = refs[5] if first_row == 0 else None
    (out_ref, mixed, summed, wide_taps) = refs[-4:]
    channels = value_ref.shape[-1]
    groups = channels // LANES
    lead = 0 if history_ref is not None else pad

    for group in range(groups):
        columns = pl.ds(group * LANES, LANES)
        wide_taps[group, :tap_count] = taps_ref[:, columns].astype(jnp.float32)
        if history_ref is not None:
            live = lax.axis_index("sp") > 0
            mixed[group, :pad] = jnp.where(live, history_ref[:, columns].astype(jnp.float32), 0.0)

    gate_rows = 32

    @pl.loop(0, (rows + lead) // gate_rows)
    def _(block):
        base = pl.multiple_of(block * gate_rows, gate_rows)
        for group in range(groups):
            columns = pl.ds(group * LANES, LANES)
            span = pl.ds(base + (first_row - lead), gate_rows)
            value = value_ref[0, span, columns].astype(jnp.float32)
            gate = gate_ref[0, span, columns].astype(jnp.float32)
            mixed[group, pl.ds(base + (pad - lead), gate_rows)] = logistic_times(value, gate)

    offset = pad - (tap_count - 1)
    step_rows = next(count for count in (64, 32) if rows % count == 0)
    tiles = step_rows // 8

    @pl.loop(0, groups)
    def _(group):
        taps = [
            jnp.broadcast_to(wide_taps[group, pl.ds(tap, 1)], (8, LANES)) for tap in range(tap_count)
        ]

        @pl.loop(0, rows // step_rows)
        def _(block):
            base = pl.multiple_of(block * step_rows, step_rows)
            totals = [None] * tiles
            for shift in range(8 * (tiles - 1) + tap_count):
                piece = mixed[group, pl.ds(base + offset + shift, 8)]
                for tile in range(tiles):
                    tap = shift - 8 * tile
                    if 0 <= tap < tap_count:
                        term = piece * taps[tap]
                        totals[tile] = term if totals[tile] is None else totals[tile] + term
                        if tap == tap_count - 1:
                            summed[group, pl.ds(base + 8 * tile, 8)] = totals[tile]

    place = lax.axis_index("dp")
    even = GATHERED[0] + tuple(offset ^ 1 for offset in GATHERED[1])
    odd = GATHERED[1] + tuple(offset ^ 1 for offset in GATHERED[0])
    per_slot = depth // LANES
    norm_rows = 16

    @pl.loop(0, rows // norm_rows)
    def _(block):
        span = pl.ds(pl.multiple_of(block * norm_rows, norm_rows), norm_rows)
        total = summed[0, span]
        for group in range(1, groups):
            total = total + summed[group, span]
        mean = jnp.sum(total, axis=-1, keepdims=True) / channels
        square = None
        for group in range(groups):
            apart = summed[group, span] - mean
            square = apart * apart if square is None else square + apart * apart
        variance = jnp.sum(square, axis=-1, keepdims=True) / channels
        scale = lax.rsqrt(variance + EPSILON)
        for slot in range(len(even)):
            owner = place ^ jnp.where(place % 2 == 0, even[slot], odd[slot])
            for part in range(per_slot):
                group = owner * per_slot + part
                normed = (summed[group, span] - mean) * scale * gain_ref[group] + shift_ref[group]
                active = logistic_times(normed, normed)
                out_ref[slot, span, pl.ds(part * LANES, LANES)] = active.astype(jnp.bfloat16)


def projected(acts, weights):
    total, slot = (None, 0)
    for weight in weights:
        for index in range(weight.shape[0]):
            left = jnp.concatenate([act[slot] for act in acts], 0)
            term = jnp.dot(left, weight[index], preferred_element_type=jnp.float32)
            total = term if total is None else total + term
            slot += 1
    return total.astype(jnp.bfloat16)


def project_kernel(chunks, *refs):
    refs[-1][...] = projected(refs[:chunks], refs[chunks:-1])


def last_kernel(chunks, layers, *refs):
    done = refs[: layers - 1]
    acts, weights = (refs[layers - 1 : layers - 1 + chunks], refs[layers - 1 + chunks : -3])
    out_ref, buf, sem = refs[-3:]
    width = buf.shape[1]
    here = lax.axis_index("sp")
    copies = []
    for step in range(layers):
        if step == layers - 1:
            buf[...] = projected(acts, weights)
        column = pl.ds(pl.multiple_of((here ^ step) * width, width), width)
        copy = pltpu.make_async_copy(
            buf if step == layers - 1 else done[step], out_ref.at[0, :, column], sem.at[step]
        )
        copy.start()
        copies.append(copy)
    for copy in copies:
        copy.wait()


VMEM = pl.BlockSpec(memory_space=pltpu.VMEM)
ANY = pl.BlockSpec(memory_space=pl.ANY)


def kernel_call(body, operands, shape, scratch=(), out_spec=VMEM, flops=0, mib=8):
    return pl.pallas_call(
        body,
        out_shape=jax.ShapeDtypeStruct(shape, jnp.bfloat16),
        in_specs=[VMEM] * len(operands),
        out_specs=out_spec,
        scratch_shapes=list(scratch),
        compiler_params=pltpu.CompilerParams(vmem_limit_bytes=mib << 20),
        cost_estimate=pl.CostEstimate(flops=flops, bytes_accessed=0, transcendentals=0),
    )(*operands)


def square_plane(value_half, gate_half, conv_taps, norm_gain, norm_shift, out_weight):
    tap_count = conv_taps.shape[0]
    tok_rows, channels = value_half.shape[1:]
    layers = lax.axis_size("sp")
    depth, width = out_weight.shape
    pad = -(-(tap_count - 1) // 32) * 32
    chunks = next(count for count in (3, 2, 4, 1) if tok_rows % (32 * count) == 0)
    rows = tok_rows // chunks
    groups = channels // LANES

    tail = kernel_call(tail_kernel, (value_half, gate_half), (pad, channels), mib=4)
    history = lax.ppermute(
        tail, "sp", [(source, (source + 1) % layers) for source in range(layers)]
    )

    gathered = []
    for step in range(layers):
        piece = named(out_weight, "sp", step, step) if step else out_weight
        first = named(piece, "dp", 2, 4)
        second = named(piece, "dp", 4, 2)
        forwarded = named(first, "dp", 4, 2)
        pieces = (piece, first, second, forwarded)
        partner = []
        for members in SWAPS[step]:
            sent = pieces[members[0]][None]
            if len(members) > 1:
                sent = kernel_call(
                    stack_kernel,
                    [pieces[member] for member in members],
                    (len(members), depth, width),
                    mib=4,
                )
            partner.append(named(sent, "dp", 1, 1))
        gathered.append([part[None] for part in pieces] + partner)

    gain, shift = (norm_gain.reshape(groups, 1, LANES), norm_shift.reshape(groups, 1, LANES))
    acts = []
    for chunk in range(chunks):
        first_row = chunk * rows
        operands = [value_half, gate_half, conv_taps, gain, shift]
        if chunk == 0:
            operands.append(history)
        acts.append(
            kernel_call(
                functools.partial(mix_kernel, first_row, rows, pad, tap_count, depth),
                operands,
                (channels // depth, rows, depth),
                (
                    pltpu.VMEM((groups, rows + pad, LANES), jnp.float32),
                    pltpu.VMEM((groups, rows, LANES), jnp.float32),
                    pltpu.VMEM((groups, -(-tap_count // 8) * 8, LANES), jnp.float32),
                ),
                flops=2 * tap_count * rows * channels,
            )
        )

    flops = 2 * tok_rows * channels * width
    done = []
    for step in range(layers - 1):
        done.append(
            kernel_call(
                functools.partial(project_kernel, chunks),
                acts + gathered[step],
                (tok_rows, width),
                flops=flops,
            )
        )
    return kernel_call(
        functools.partial(last_kernel, chunks, layers),
        done + acts + gathered[layers - 1],
        (1, tok_rows, layers * width),
        (pltpu.VMEM((tok_rows, width), jnp.bfloat16), pltpu.SemaphoreType.DMA((layers,))),
        out_spec=ANY,
        flops=flops,
    )


def solution(mesh):
    placed = (P("dp", "sp", None), P("dp", "sp", None), P(), P(), P(), P("dp", "sp"))
    plain = mesh.shape["dp"] != 8 or mesh.shape["sp"] != 4

    def per_device(*operands):
        if plain:
            return general(*operands)
        return square_plane(*operands)

    return jax.shard_map(
        per_device, mesh=mesh, in_specs=placed, out_specs=P("dp", "sp", None), check_vma=False
    )
```

```python
import functools

import jax
import jax.numpy as jnp
from jax import lax
from jax.experimental import pallas as pl
from jax.experimental.pallas import tpu as pltpu
from jax.sharding import PartitionSpec as P


EPSILON = 1e-06
LANES = 128


def swapped(value, axis, mask_of):
    count = lax.axis_size(axis)
    return lax.ppermute(value, axis, [(index, index ^ mask_of(index)) for index in range(count)])


def named(value, axis, even, odd):
    return swapped(value, axis, lambda index: odd if index & 1 else even)


def passed_along(value, axis, steps):
    count = lax.axis_size(axis)
    initial, last = (max(0, -steps), min(count, count - steps))
    return lax.ppermute(value, axis, [(source, source + steps) for source in range(initial, last)])


def plane_gather(piece, axis):
    count = lax.axis_size(axis)
    masks = [1 << bit for bit in range(1, (count - 1).bit_length())]
    held = piece[None]
    for even, odd in zip(masks, masks[::-1]):
        other = swapped(held, axis, lambda index: odd if index & 1 else even)
        held = jnp.concatenate([held, other], 0)
    return jnp.concatenate([held, swapped(held, axis, lambda index: 1)], 0)


def slot_offsets(count):
    masks = [1 << bit for bit in range(1, (count - 1).bit_length())]
    halves = []
    for order in (masks, masks[::-1]):
        held = [0]
        for mask in order:
            held = held + [offset ^ mask for offset in held]
        halves.append(held)
    return [halves[parity] + [offset ^ 1 for offset in halves[1 - parity]] for parity in range(2)]


def general(value_half, gate_half, conv_taps, norm_gain, norm_shift, out_weight):
    tap_count, tok_rows = (conv_taps.shape[0], value_half.shape[1])
    layers, blocks = (lax.axis_size("sp"), lax.axis_size("dp"))
    here, place = (lax.axis_index("sp"), lax.axis_index("dp"))
    depth, width = out_weight.shape
    gathered = [
        plane_gather(swapped(out_weight, "sp", lambda index: step) if step else out_weight, "dp")
        for step in range(layers)
    ]
    gated = (
        value_half[0].astype(jnp.float32) * jax.nn.sigmoid(gate_half[0].astype(jnp.float32))
    ).astype(jnp.bfloat16)
    history = passed_along(gated[tok_rows - (tap_count - 1) :], "sp", 1)
    padded = jnp.concatenate([history, gated], 0)
    running = jnp.zeros(gated.shape, jnp.float32)
    for tap_index in range(tap_count):
        running = running + padded[tap_index : tap_index + tok_rows].astype(jnp.float32) * conv_taps[
            tap_index
        ].astype(jnp.float32)
    widened = running.astype(jnp.bfloat16).astype(jnp.float32)
    centered = widened - jnp.mean(widened, axis=-1, keepdims=True)
    variance = jnp.mean(centered * centered, axis=-1, keepdims=True)
    normed = centered * lax.rsqrt(variance + EPSILON) * norm_gain + norm_shift
    activated = jax.nn.silu(normed).astype(jnp.bfloat16)
    even, odd = slot_offsets(blocks)
    offsets = jnp.where(place % 2 == 0, jnp.array(even), jnp.array(odd))
    ordered = jnp.concatenate(
        [
            lax.dynamic_slice_in_dim(activated, (place ^ offsets[slot]) * depth, depth, 1)
            for slot in range(blocks)
        ],
        1,
    )
    out = jnp.zeros((tok_rows, layers * width), jnp.bfloat16)
    for step in range(layers):
        part = jnp.dot(
            ordered,
            gathered[step].reshape(blocks * depth, width),
            preferred_element_type=jnp.float32,
        ).astype(jnp.bfloat16)
        out = lax.dynamic_update_slice_in_dim(out, part, (here ^ step) * width, 1)
    return out[None]


GATHERED = ((0, 2, 4, 6), (0, 4, 2, 6))


def logistic_times(value, argument):
    return value / (1.0 + jnp.exp(-argument))


def blank_kernel(out_ref):
    out_ref[...] = jnp.zeros_like(out_ref)


def gate_kernel(pad, tap_count, *refs):
    (value_ref, gate_ref, taps_ref) = refs[:3]
    (mixed, tail_ref, wide_taps) = refs[-3:]
    (rows, channels) = value_ref.shape[1:]
    groups = channels // LANES
    gate_rows = 32

    @pl.loop(0, rows // gate_rows)
    def _(block):
        span = pl.ds(pl.multiple_of(block * gate_rows, gate_rows), gate_rows)
        for group in range(groups):
            columns = pl.ds(group * LANES, LANES)
            value = value_ref[0, span, columns].astype(jnp.float32)
            gate = gate_ref[0, span, columns].astype(jnp.float32)
            gated = logistic_times(value, gate).astype(jnp.bfloat16)
            mixed[group, span] = gated.astype(jnp.float32)

    for group in range(groups):
        columns = pl.ds(group * LANES, LANES)
        tail_ref[:, columns] = mixed[group, pl.ds(rows - pad, pad)].astype(jnp.bfloat16)
    for group in range(groups):
        wide_taps[group, :tap_count] = taps_ref[:, pl.ds(group * LANES, LANES)].astype(jnp.float32)


def stack_kernel(*refs):
    for index, ref in enumerate(refs[:-1]):
        refs[-1][index] = ref[...]


def mix_kernel(first_row, rows, pad, tap_count, depth, *refs):
    (mixed, wide_taps, gain_ref, shift_ref) = refs[:4]
    if first_row == 0:
        (history_ref, out_ref, summed, total, scale_ref, shown) = refs[4:]
    else:
        (out_ref, summed, total, scale_ref) = refs[4:]
        shown = mixed
    groups = mixed.shape[0]
    channels = groups * LANES
    if first_row == 0:
        live = lax.axis_index("sp") > 0
        for group in range(groups):
            columns = pl.ds(group * LANES, LANES)
            shown[group, :pad] = jnp.where(live, history_ref[:, columns].astype(jnp.float32), 0.0)
            shown[group, pl.ds(pad, rows)] = mixed[group, :rows]
    offset = (pad if first_row == 0 else first_row) - (tap_count - 1)
    tiles = rows // 8
    total[...] = jnp.zeros_like(total)

    @pl.loop(0, groups)
    def _(group):
        taps = [
            jnp.broadcast_to(wide_taps[group, pl.ds(tap, 1)], (8, LANES)) for tap in range(tap_count)
        ]
        totals = [None] * tiles
        for shift in range(8 * (tiles - 1) + tap_count):
            piece = shown[group, pl.ds(offset + shift, 8)]
            for tile in range(tiles):
                tap = shift - 8 * tile
                if 0 <= tap < tap_count:
                    term = piece * taps[tap]
                    totals[tile] = term if totals[tile] is None else totals[tile] + term
                    if tap == tap_count - 1:
                        rounded = totals[tile].astype(jnp.bfloat16).astype(jnp.float32)
                        summed[group, pl.ds(8 * tile, 8)] = rounded
                        total[pl.ds(8 * tile, 8)] += rounded

    mean = jnp.sum(total[...], axis=-1, keepdims=True) / channels
    total[...] = jnp.broadcast_to(mean, total.shape)
    norm_rows = 16

    @pl.loop(0, rows // norm_rows)
    def _(block):
        span = pl.ds(pl.multiple_of(block * norm_rows, norm_rows), norm_rows)
        square = None
        for group in range(groups):
            apart = summed[group, span] - total[span]
            square = apart * apart if square is None else square + apart * apart
        scale_ref[span] = square

    variance = jnp.sum(scale_ref[...], axis=-1, keepdims=True) / channels
    scale_ref[...] = jnp.broadcast_to(lax.rsqrt(variance + EPSILON), scale_ref.shape)

    place = lax.axis_index("dp")
    even = GATHERED[0] + tuple(offset ^ 1 for offset in GATHERED[1])
    odd = GATHERED[1] + tuple(offset ^ 1 for offset in GATHERED[0])
    per_slot = depth // LANES

    @pl.loop(0, rows // norm_rows)
    def _(block):
        span = pl.ds(pl.multiple_of(block * norm_rows, norm_rows), norm_rows)
        for slot in range(len(even)):
            owner = place ^ jnp.where(place % 2 == 0, even[slot], odd[slot])
            for part in range(per_slot):
                group = owner * per_slot + part
                normed = (summed[group, span] - total[span]) * scale_ref[span]
                normed = normed * gain_ref[group] + shift_ref[group]
                active = logistic_times(normed, normed)
                out_ref[slot, span, pl.ds(part * LANES, LANES)] = active.astype(jnp.bfloat16)


def projected(acts, weights, slots):
    total = None
    for weight, places in zip(weights, slots, strict=True):
        for index, slot in enumerate(places):
            left = jnp.concatenate([act[slot] for act in acts], 0)
            term = jnp.dot(left, weight[index], preferred_element_type=jnp.float32)
            total = term if total is None else total + term
    return total


def project_kernel(chunks, slots, *refs):
    refs[-1][...] = projected(refs[:chunks], refs[chunks:-1], slots).astype(refs[-1].dtype)


def last_kernel(chunks, slots, *refs):
    (begun, done) = (refs[0], refs[1:4])
    (acts, weights) = (refs[4 : 4 + chunks], refs[4 + chunks : -3])
    (out_ref, buf, sem) = refs[-3:]
    width = buf.shape[1]
    (here, parity) = (lax.axis_index("sp"), lax.axis_index("dp") % 2)
    copies = []
    for index, step in enumerate((0, 1 + parity, 2 - parity, 3)):
        if index == len(done):
            buf[...] = (begun[...] + projected(acts, weights, slots)).astype(buf.dtype)
        column = pl.ds(pl.multiple_of((here ^ step) * width, width), width)
        source = buf if index == len(done) else done[index]
        copy = pltpu.make_async_copy(source, out_ref.at[0, :, column], sem.at[index])
        copy.start()
        copies.append(copy)
    for copy in copies:
        copy.wait()


VMEM = pl.BlockSpec(memory_space=pltpu.VMEM)
ANY = pl.BlockSpec(memory_space=pl.ANY)


HBM = pl.BlockSpec(memory_space=pltpu.HBM)


def kernel_call(body, operands, outs, scratch=(), out_spec=VMEM, flops=0, mib=8, hbm=0):
    outs = [jax.ShapeDtypeStruct(out, jnp.bfloat16) if isinstance(out, tuple) else out for out in outs]
    results = pl.pallas_call(
        body,
        out_shape=outs,
        in_specs=[HBM] * hbm + [VMEM] * (len(operands) - hbm),
        out_specs=[out_spec] * len(outs),
        scratch_shapes=list(scratch),
        compiler_params=pltpu.CompilerParams(vmem_limit_bytes=mib << 20),
        cost_estimate=pl.CostEstimate(flops=flops, bytes_accessed=0, transcendentals=0),
    )(*operands)
    return results if len(outs) > 1 else results[0]


def square_plane(value_half, gate_half, conv_taps, norm_gain, norm_shift, out_weight):
    tap_count = conv_taps.shape[0]
    tok_rows, channels = value_half.shape[1:]
    layers = lax.axis_size("sp")
    depth, width = out_weight.shape
    pad = -(-(tap_count - 1) // 32) * 32
    rows = next(count for count in (64, 64, 32) if tok_rows % count == 0)
    chunks = tok_rows // rows
    groups = channels // LANES

    gain, shift = (norm_gain.reshape(groups, 1, LANES), norm_shift.reshape(groups, 1, LANES))
    blank = kernel_call(blank_kernel, (), [(16, LANES)], flops=1 << 36)
    mixed, tail, taps = kernel_call(
        functools.partial(gate_kernel, pad, tap_count),
        (value_half, gate_half, conv_taps, blank),
        (
            jax.ShapeDtypeStruct((groups, tok_rows, LANES), jnp.float32),
            (pad, channels),
            jax.ShapeDtypeStruct((groups, -(-tap_count // 8) * 8, LANES), jnp.float32),
        ),
        flops=40 * tok_rows * channels,
        mib=8,
    )
    history = lax.ppermute(
        tail, "sp", [(source, (source + 1) % layers) for source in range(layers)]
    )

    def both(pieces):
        stacked = kernel_call(stack_kernel, pieces, [(len(pieces), depth, width)], mib=4)
        return named(stacked, "dp", 1, 1)

    singles = []
    for step in (0, 3):
        if step:
            piece = named(out_weight, "sp", 3, 3)
            partner = named(piece, "dp", 1, 1)
        else:
            piece = out_weight
            partner = own_partner = named(out_weight, "dp", 1, 1)
        first = named(piece, "dp", 2, 4)
        second = named(piece, "dp", 4, 2)
        forwarded = named(first, "dp", 4, 2)
        singles.append((piece, first, second, forwarded, partner))

    chip = kernel_call(stack_kernel, (out_weight, own_partner), [(2, depth, width)], mib=4)
    blocks = lax.axis_size("dp")
    route = [
        (z * blocks + d, (z ^ (2 if d % 2 else 1)) * blocks + d)
        for z in range(layers)
        for d in range(blocks)
    ]
    arrived = lax.ppermute(chip, ("sp", "dp"), route)
    first = named(arrived, "dp", 2, 4)
    second = named(arrived, "dp", 4, 2)
    forwarded = named(first, "dp", 4, 2)
    pairs = (arrived, first, second, forwarded)
    pairs_other = [named(pair, "dp", 1, 1) for pair in pairs]

    acts = []
    for chunk in range(chunks):
        operands = [mixed, taps, gain, shift]
        scratch = [
            pltpu.VMEM((groups, rows, LANES), jnp.float32),
            pltpu.VMEM((rows, LANES), jnp.float32),
            pltpu.VMEM((rows, LANES), jnp.float32),
        ]
        if chunk == 0:
            operands.append(history)
            scratch.append(pltpu.VMEM((groups, rows + pad, LANES), jnp.float32))
        acts.append(
            kernel_call(
                functools.partial(mix_kernel, chunk * rows, rows, pad, tap_count, depth),
                operands,
                [(channels // depth, rows, depth)],
                scratch,
                flops=2 * tap_count * rows * channels,
            )
        )

    def project(weights, slots, dtype=jnp.bfloat16):
        weights = [weight if weight.ndim == 3 else weight[None] for weight in weights]
        return kernel_call(
            functools.partial(project_kernel, chunks, slots),
            acts + weights,
            [jax.ShapeDtypeStruct((tok_rows, width), dtype)],
            flops=2 * tok_rows * depth * width * sum(len(places) for places in slots),
        )

    (piece, first, second, forwarded, partner) = singles[0]
    swapped_0 = both((first, second, forwarded))
    done = [
        project(
            (piece, first, second, forwarded, partner, swapped_0),
            ((0,), (1,), (2,), (3,), (4,), (5, 6, 7)),
        ),
        project(pairs, ((0, 4), (1, 6), (2, 5), (3, 7))),
        project(pairs_other, ((4, 0), (5, 2), (6, 1), (7, 3))),
    ]
    (piece, first, second, forwarded, partner) = singles[1]
    swapped_3 = both((first, second))
    begun = project(
        (piece, first, second, partner, swapped_3), ((0,), (1,), (2,), (4,), (5, 6)), jnp.float32
    )
    last = named(forwarded, "dp", 1, 1)
    return kernel_call(
        functools.partial(last_kernel, chunks, ((3,), (7,))),
        [begun] + done + acts + [forwarded[None], last[None]],
        [(1, tok_rows, layers * width)],
        (pltpu.VMEM((tok_rows, width), jnp.bfloat16), pltpu.SemaphoreType.DMA((layers,))),
        out_spec=ANY,
        flops=4 * tok_rows * depth * width,
    )


def solution(mesh):
    placed = (P("dp", "sp", None), P("dp", "sp", None), P(), P(), P(), P("dp", "sp"))
    plain = mesh.shape["dp"] != 8 or mesh.shape["sp"] != 4

    def per_device(*operands):
        if plain:
            return general(*operands)
        return square_plane(*operands)

    return jax.shard_map(
        per_device, mesh=mesh, in_specs=placed, out_specs=P("dp", "sp", None), check_vma=False
    )
```

```python
import functools

import jax
import jax.numpy as jnp
from jax import lax
from jax.experimental import pallas as pl
from jax.experimental.pallas import tpu as pltpu
from jax.sharding import PartitionSpec as P


EPSILON = 1e-06
LANES = 128


def swapped(value, axis, mask_of):
    count = lax.axis_size(axis)
    return lax.ppermute(value, axis, [(index, index ^ mask_of(index)) for index in range(count)])


def named(value, axis, even, odd):
    return swapped(value, axis, lambda index: odd if index & 1 else even)


def passed_along(value, axis, steps):
    count = lax.axis_size(axis)
    initial, last = (max(0, -steps), min(count, count - steps))
    return lax.ppermute(value, axis, [(source, source + steps) for source in range(initial, last)])


def plane_gather(piece, axis):
    count = lax.axis_size(axis)
    masks = [1 << bit for bit in range(1, (count - 1).bit_length())]
    held = piece[None]
    for even, odd in zip(masks, masks[::-1]):
        other = swapped(held, axis, lambda index: odd if index & 1 else even)
        held = jnp.concatenate([held, other], 0)
    return jnp.concatenate([held, swapped(held, axis, lambda index: 1)], 0)


def slot_offsets(count):
    masks = [1 << bit for bit in range(1, (count - 1).bit_length())]
    halves = []
    for order in (masks, masks[::-1]):
        held = [0]
        for mask in order:
            held = held + [offset ^ mask for offset in held]
        halves.append(held)
    return [halves[parity] + [offset ^ 1 for offset in halves[1 - parity]] for parity in range(2)]


def general(value_half, gate_half, conv_taps, norm_gain, norm_shift, out_weight):
    tap_count, tok_rows = (conv_taps.shape[0], value_half.shape[1])
    layers, blocks = (lax.axis_size("sp"), lax.axis_size("dp"))
    here, place = (lax.axis_index("sp"), lax.axis_index("dp"))
    depth, width = out_weight.shape
    gathered = [
        plane_gather(swapped(out_weight, "sp", lambda index: step) if step else out_weight, "dp")
        for step in range(layers)
    ]
    gated = (
        value_half[0].astype(jnp.float32) * jax.nn.sigmoid(gate_half[0].astype(jnp.float32))
    ).astype(jnp.bfloat16)
    history = passed_along(gated[tok_rows - (tap_count - 1) :], "sp", 1)
    padded = jnp.concatenate([history, gated], 0)
    running = jnp.zeros(gated.shape, jnp.float32)
    for tap_index in range(tap_count):
        running = running + padded[tap_index : tap_index + tok_rows].astype(jnp.float32) * conv_taps[
            tap_index
        ].astype(jnp.float32)
    widened = running.astype(jnp.bfloat16).astype(jnp.float32)
    centered = widened - jnp.mean(widened, axis=-1, keepdims=True)
    variance = jnp.mean(centered * centered, axis=-1, keepdims=True)
    normed = centered * lax.rsqrt(variance + EPSILON) * norm_gain + norm_shift
    activated = jax.nn.silu(normed).astype(jnp.bfloat16)
    even, odd = slot_offsets(blocks)
    offsets = jnp.where(place % 2 == 0, jnp.array(even), jnp.array(odd))
    ordered = jnp.concatenate(
        [
            lax.dynamic_slice_in_dim(activated, (place ^ offsets[slot]) * depth, depth, 1)
            for slot in range(blocks)
        ],
        1,
    )
    out = jnp.zeros((tok_rows, layers * width), jnp.bfloat16)
    for step in range(layers):
        part = jnp.dot(
            ordered,
            gathered[step].reshape(blocks * depth, width),
            preferred_element_type=jnp.float32,
        ).astype(jnp.bfloat16)
        out = lax.dynamic_update_slice_in_dim(out, part, (here ^ step) * width, 1)
    return out[None]


GATHERED = ((0, 2, 4, 6), (0, 4, 2, 6))


def logistic_times(value, argument):
    return value / (1.0 + jnp.exp(-argument))


def blank_kernel(out_ref):
    out_ref[...] = jnp.zeros_like(out_ref)


def gate_kernel(pad, tap_count, *refs):
    (value_ref, gate_ref, taps_ref) = refs[:3]
    (mixed, tail_ref, wide_taps) = refs[-3:]
    (rows, channels) = value_ref.shape[1:]
    groups = channels // LANES
    gate_rows = 32

    @pl.loop(0, rows // gate_rows)
    def _(block):
        span = pl.ds(pl.multiple_of(block * gate_rows, gate_rows), gate_rows)
        for group in range(groups):
            columns = pl.ds(group * LANES, LANES)
            value = value_ref[0, span, columns].astype(jnp.float32)
            gate = gate_ref[0, span, columns].astype(jnp.float32)
            gated = logistic_times(value, gate).astype(jnp.bfloat16)
            mixed[group, span] = gated.astype(jnp.float32)

    for group in range(groups):
        columns = pl.ds(group * LANES, LANES)
        tail_ref[:, columns] = mixed[group, pl.ds(rows - pad, pad)].astype(jnp.bfloat16)
    for group in range(groups):
        wide_taps[group, :tap_count] = taps_ref[:, pl.ds(group * LANES, LANES)].astype(jnp.float32)


def stack_kernel(*refs):
    for index, ref in enumerate(refs[:-1]):
        refs[-1][index] = ref[...]


def mix_kernel(first_row, rows, pad, tap_count, depth, *refs):
    (mixed, wide_taps, gain_ref, shift_ref) = refs[:4]
    if first_row == 0:
        (history_ref, out_ref, summed, total, scale_ref, shown) = refs[4:]
    else:
        (out_ref, summed, total, scale_ref) = refs[4:]
        shown = mixed
    groups = mixed.shape[0]
    channels = groups * LANES
    if first_row == 0:
        live = lax.axis_index("sp") > 0
        for group in range(groups):
            columns = pl.ds(group * LANES, LANES)
            shown[group, :pad] = jnp.where(live, history_ref[:, columns].astype(jnp.float32), 0.0)
            shown[group, pl.ds(pad, rows)] = mixed[group, :rows]
    offset = (pad if first_row == 0 else first_row) - (tap_count - 1)
    tiles = rows // 8
    total[...] = jnp.zeros_like(total)

    @pl.loop(0, groups)
    def _(group):
        taps = [
            jnp.broadcast_to(wide_taps[group, pl.ds(tap, 1)], (8, LANES)) for tap in range(tap_count)
        ]
        totals = [None] * tiles
        for shift in range(8 * (tiles - 1) + tap_count):
            piece = shown[group, pl.ds(offset + shift, 8)]
            for tile in range(tiles):
                tap = shift - 8 * tile
                if 0 <= tap < tap_count:
                    term = piece * taps[tap]
                    totals[tile] = term if totals[tile] is None else totals[tile] + term
                    if tap == tap_count - 1:
                        rounded = totals[tile].astype(jnp.bfloat16).astype(jnp.float32)
                        summed[group, pl.ds(8 * tile, 8)] = rounded
                        total[pl.ds(8 * tile, 8)] += rounded

    mean = jnp.sum(total[...], axis=-1, keepdims=True) / channels
    total[...] = jnp.broadcast_to(mean, total.shape)
    norm_rows = 16

    @pl.loop(0, rows // norm_rows)
    def _(block):
        span = pl.ds(pl.multiple_of(block * norm_rows, norm_rows), norm_rows)
        square = None
        for group in range(groups):
            apart = summed[group, span] - total[span]
            square = apart * apart if square is None else square + apart * apart
        scale_ref[span] = square

    variance = jnp.sum(scale_ref[...], axis=-1, keepdims=True) / channels
    scale_ref[...] = jnp.broadcast_to(lax.rsqrt(variance + EPSILON), scale_ref.shape)

    place = lax.axis_index("dp")
    even = GATHERED[0] + tuple(offset ^ 1 for offset in GATHERED[1])
    odd = GATHERED[1] + tuple(offset ^ 1 for offset in GATHERED[0])
    per_slot = depth // LANES

    @pl.loop(0, rows // norm_rows)
    def _(block):
        span = pl.ds(pl.multiple_of(block * norm_rows, norm_rows), norm_rows)
        for slot in range(len(even)):
            owner = place ^ jnp.where(place % 2 == 0, even[slot], odd[slot])
            for part in range(per_slot):
                group = owner * per_slot + part
                normed = (summed[group, span] - total[span]) * scale_ref[span]
                normed = normed * gain_ref[group] + shift_ref[group]
                active = logistic_times(normed, normed)
                out_ref[slot, span, pl.ds(part * LANES, LANES)] = active.astype(jnp.bfloat16)


def projected(acts, weights, slots):
    total = None
    for weight, places in zip(weights, slots, strict=True):
        for index, slot in enumerate(places):
            left = jnp.concatenate([act[slot] for act in acts], 0)
            term = jnp.dot(left, weight[index], preferred_element_type=jnp.float32)
            total = term if total is None else total + term
    return total


def project_kernel(chunks, slots, *refs):
    refs[-1][...] = projected(refs[:chunks], refs[chunks:-1], slots).astype(refs[-1].dtype)


def last_kernel(chunks, slots, *refs):
    (begun, done) = (refs[0], refs[1:4])
    (acts, weights) = (refs[4 : 4 + chunks], refs[4 + chunks : -3])
    (out_ref, buf, sem) = refs[-3:]
    width = buf.shape[1]
    (here, parity) = (lax.axis_index("sp"), lax.axis_index("dp") % 2)
    copies = []
    for index, step in enumerate((0, 1 + parity, 2 - parity, 3)):
        if index == len(done):
            buf[...] = (begun[...] + projected(acts, weights, slots)).astype(buf.dtype)
        column = pl.ds(pl.multiple_of((here ^ step) * width, width), width)
        source = buf if index == len(done) else done[index]
        copy = pltpu.make_async_copy(source, out_ref.at[0, :, column], sem.at[index])
        copy.start()
        copies.append(copy)
    for copy in copies:
        copy.wait()


VMEM = pl.BlockSpec(memory_space=pltpu.VMEM)
ANY = pl.BlockSpec(memory_space=pl.ANY)


HBM = pl.BlockSpec(memory_space=pltpu.HBM)


def kernel_call(body, operands, outs, scratch=(), out_spec=VMEM, flops=0, mib=8, hbm=0):
    outs = [jax.ShapeDtypeStruct(out, jnp.bfloat16) if isinstance(out, tuple) else out for out in outs]
    results = pl.pallas_call(
        body,
        out_shape=outs,
        in_specs=[HBM] * hbm + [VMEM] * (len(operands) - hbm),
        out_specs=[out_spec] * len(outs),
        scratch_shapes=list(scratch),
        compiler_params=pltpu.CompilerParams(vmem_limit_bytes=mib << 20),
        cost_estimate=pl.CostEstimate(flops=flops, bytes_accessed=0, transcendentals=0),
    )(*operands)
    return results if len(outs) > 1 else results[0]


def square_plane(value_half, gate_half, conv_taps, norm_gain, norm_shift, out_weight):
    tap_count = conv_taps.shape[0]
    tok_rows, channels = value_half.shape[1:]
    layers = lax.axis_size("sp")
    depth, width = out_weight.shape
    pad = -(-(tap_count - 1) // 32) * 32
    rows = next(count for count in (64, 64, 32) if tok_rows % count == 0)
    chunks = tok_rows // rows
    groups = channels // LANES

    gain, shift = (norm_gain.reshape(groups, 1, LANES), norm_shift.reshape(groups, 1, LANES))
    blank = kernel_call(blank_kernel, (), [(16, LANES)], flops=1 << 36)
    mixed, tail, taps = kernel_call(
        functools.partial(gate_kernel, pad, tap_count),
        (value_half, gate_half, conv_taps, blank),
        (
            jax.ShapeDtypeStruct((groups, tok_rows, LANES), jnp.float32),
            (pad, channels),
            jax.ShapeDtypeStruct((groups, -(-tap_count // 8) * 8, LANES), jnp.float32),
        ),
        flops=40 * tok_rows * channels,
        mib=8,
    )
    history = lax.ppermute(
        tail, "sp", [(source, (source + 1) % layers) for source in range(layers)]
    )

    def both(pieces):
        stacked = kernel_call(stack_kernel, pieces, [(len(pieces), depth, width)], mib=4)
        return named(stacked, "dp", 1, 1)

    singles = []
    for step in (0, 3):
        if step:
            piece = named(out_weight, "sp", 3, 3)
            partner = named(piece, "dp", 1, 1)
        else:
            piece = out_weight
            partner = own_partner = named(out_weight, "dp", 1, 1)
        first = named(piece, "dp", 2, 4)
        second = named(piece, "dp", 4, 2)
        if step:
            forwarded = named(singles[0][3], "sp", step, step)
        else:
            forwarded = named(first, "dp", 4, 2)
        singles.append((piece, first, second, forwarded, partner))

    chip = kernel_call(stack_kernel, (out_weight, own_partner), [(2, depth, width)], mib=4)
    blocks = lax.axis_size("dp")
    route = [
        (z * blocks + d, (z ^ (2 if d % 2 else 1)) * blocks + d)
        for z in range(layers)
        for d in range(blocks)
    ]
    arrived = lax.ppermute(chip, ("sp", "dp"), route)
    first = named(arrived, "dp", 2, 4)
    second = named(arrived, "dp", 4, 2)
    forwarded = named(first, "dp", 4, 2)
    pairs = (arrived, first, second, forwarded)
    pairs_other = [named(pair, "dp", 1, 1) for pair in pairs]

    acts = []
    for chunk in range(chunks):
        operands = [mixed, taps, gain, shift]
        scratch = [
            pltpu.VMEM((groups, rows, LANES), jnp.float32),
            pltpu.VMEM((rows, LANES), jnp.float32),
            pltpu.VMEM((rows, LANES), jnp.float32),
        ]
        if chunk == 0:
            operands.append(history)
            scratch.append(pltpu.VMEM((groups, rows + pad, LANES), jnp.float32))
        acts.append(
            kernel_call(
                functools.partial(mix_kernel, chunk * rows, rows, pad, tap_count, depth),
                operands,
                [(channels // depth, rows, depth)],
                scratch,
                flops=2 * tap_count * rows * channels,
            )
        )

    def project(weights, slots, dtype=jnp.bfloat16):
        weights = [weight if weight.ndim == 3 else weight[None] for weight in weights]
        return kernel_call(
            functools.partial(project_kernel, chunks, slots),
            acts + weights,
            [jax.ShapeDtypeStruct((tok_rows, width), dtype)],
            flops=2 * tok_rows * depth * width * sum(len(places) for places in slots),
        )

    (piece, first, second, forwarded, partner) = singles[0]
    swapped_0 = both((first, second, forwarded))
    done = [
        project(
            (piece, first, second, forwarded, partner, swapped_0),
            ((0,), (1,), (2,), (3,), (4,), (5, 6, 7)),
        ),
        project(pairs, ((0, 4), (1, 6), (2, 5), (3, 7))),
        project(pairs_other, ((4, 0), (5, 2), (6, 1), (7, 3))),
    ]
    (piece, first, second, forwarded, partner) = singles[1]
    last = named(forwarded, "dp", 1, 1)
    begun = project((piece, partner, forwarded, last), ((0,), (4,), (3,), (7,)), jnp.float32)
    swapped_3 = both((first, second))
    return kernel_call(
        functools.partial(last_kernel, chunks, ((1,), (2,), (5, 6))),
        [begun] + done + acts + [first[None], second[None], swapped_3],
        [(1, tok_rows, layers * width)],
        (pltpu.VMEM((tok_rows, width), jnp.bfloat16), pltpu.SemaphoreType.DMA((layers,))),
        out_spec=ANY,
        flops=8 * tok_rows * depth * width,
    )


def solution(mesh):
    placed = (P("dp", "sp", None), P("dp", "sp", None), P(), P(), P(), P("dp", "sp"))
    plain = mesh.shape["dp"] != 8 or mesh.shape["sp"] != 4

    def per_device(*operands):
        if plain:
            return general(*operands)
        return square_plane(*operands)

    return jax.shard_map(
        per_device, mesh=mesh, in_specs=placed, out_specs=P("dp", "sp", None), check_vma=False
    )
```

```python
import functools

import jax
import jax.numpy as jnp
from jax import lax
from jax.experimental import pallas as pl
from jax.experimental.pallas import tpu as pltpu
from jax.sharding import PartitionSpec as P


EPSILON = 1e-06
LANES = 128


def swapped(value, axis, mask_of):
    count = lax.axis_size(axis)
    return lax.ppermute(value, axis, [(index, index ^ mask_of(index)) for index in range(count)])


def named(value, axis, even, odd):
    return swapped(value, axis, lambda index: odd if index & 1 else even)


def passed_along(value, axis, steps):
    count = lax.axis_size(axis)
    initial, last = (max(0, -steps), min(count, count - steps))
    return lax.ppermute(value, axis, [(source, source + steps) for source in range(initial, last)])


def plane_gather(piece, axis):
    count = lax.axis_size(axis)
    masks = [1 << bit for bit in range(1, (count - 1).bit_length())]
    held = piece[None]
    for even, odd in zip(masks, masks[::-1]):
        other = swapped(held, axis, lambda index: odd if index & 1 else even)
        held = jnp.concatenate([held, other], 0)
    return jnp.concatenate([held, swapped(held, axis, lambda index: 1)], 0)


def slot_offsets(count):
    masks = [1 << bit for bit in range(1, (count - 1).bit_length())]
    halves = []
    for order in (masks, masks[::-1]):
        held = [0]
        for mask in order:
            held = held + [offset ^ mask for offset in held]
        halves.append(held)
    return [halves[parity] + [offset ^ 1 for offset in halves[1 - parity]] for parity in range(2)]


def general(value_half, gate_half, conv_taps, norm_gain, norm_shift, out_weight):
    tap_count, tok_rows = (conv_taps.shape[0], value_half.shape[1])
    layers, blocks = (lax.axis_size("sp"), lax.axis_size("dp"))
    here, place = (lax.axis_index("sp"), lax.axis_index("dp"))
    depth, width = out_weight.shape
    gathered = [
        plane_gather(swapped(out_weight, "sp", lambda index: step) if step else out_weight, "dp")
        for step in range(layers)
    ]
    gated = (
        value_half[0].astype(jnp.float32) * jax.nn.sigmoid(gate_half[0].astype(jnp.float32))
    ).astype(jnp.bfloat16)
    history = passed_along(gated[tok_rows - (tap_count - 1) :], "sp", 1)
    padded = jnp.concatenate([history, gated], 0)
    running = jnp.zeros(gated.shape, jnp.float32)
    for tap_index in range(tap_count):
        running = running + padded[tap_index : tap_index + tok_rows].astype(jnp.float32) * conv_taps[
            tap_index
        ].astype(jnp.float32)
    widened = running.astype(jnp.bfloat16).astype(jnp.float32)
    centered = widened - jnp.mean(widened, axis=-1, keepdims=True)
    variance = jnp.mean(centered * centered, axis=-1, keepdims=True)
    normed = centered * lax.rsqrt(variance + EPSILON) * norm_gain + norm_shift
    activated = jax.nn.silu(normed).astype(jnp.bfloat16)
    even, odd = slot_offsets(blocks)
    offsets = jnp.where(place % 2 == 0, jnp.array(even), jnp.array(odd))
    ordered = jnp.concatenate(
        [
            lax.dynamic_slice_in_dim(activated, (place ^ offsets[slot]) * depth, depth, 1)
            for slot in range(blocks)
        ],
        1,
    )
    out = jnp.zeros((tok_rows, layers * width), jnp.bfloat16)
    for step in range(layers):
        part = jnp.dot(
            ordered,
            gathered[step].reshape(blocks * depth, width),
            preferred_element_type=jnp.float32,
        ).astype(jnp.bfloat16)
        out = lax.dynamic_update_slice_in_dim(out, part, (here ^ step) * width, 1)
    return out[None]


GATHERED = ((0, 2, 4, 6), (0, 4, 2, 6))


def logistic_times(value, argument):
    return value / (1.0 + jnp.exp(-argument))


def blank_kernel(out_ref):
    out_ref[...] = jnp.zeros_like(out_ref)


def gate_kernel(pad, tap_count, *refs):
    (value_ref, gate_ref, taps_ref) = refs[:3]
    (mixed, tail_ref, wide_taps) = refs[-3:]
    (rows, channels) = value_ref.shape[1:]
    groups = channels // LANES
    gate_rows = 32

    @pl.loop(0, rows // gate_rows)
    def _(block):
        span = pl.ds(pl.multiple_of(block * gate_rows, gate_rows), gate_rows)
        for group in range(groups):
            columns = pl.ds(group * LANES, LANES)
            value = value_ref[0, span, columns].astype(jnp.float32)
            gate = gate_ref[0, span, columns].astype(jnp.float32)
            gated = logistic_times(value, gate).astype(jnp.bfloat16)
            mixed[group, span] = gated.astype(jnp.float32)

    for group in range(groups):
        columns = pl.ds(group * LANES, LANES)
        tail_ref[:, columns] = mixed[group, pl.ds(rows - pad, pad)].astype(jnp.bfloat16)
    for group in range(groups):
        wide_taps[group, :tap_count] = taps_ref[:, pl.ds(group * LANES, LANES)].astype(jnp.float32)


def stack_kernel(*refs):
    for index, ref in enumerate(refs[:-1]):
        refs[-1][index] = ref[...]


def mix_kernel(first_row, rows, pad, tap_count, depth, *refs):
    (mixed, wide_taps, gain_ref, shift_ref) = refs[:4]
    if first_row == 0:
        (history_ref, out_ref, summed, total, scale_ref, shown) = refs[4:]
    else:
        (out_ref, summed, total, scale_ref) = refs[4:]
        shown = mixed
    groups = mixed.shape[0]
    channels = groups * LANES
    if first_row == 0:
        live = lax.axis_index("sp") > 0
        for group in range(groups):
            columns = pl.ds(group * LANES, LANES)
            shown[group, :pad] = jnp.where(live, history_ref[:, columns].astype(jnp.float32), 0.0)
            shown[group, pl.ds(pad, rows)] = mixed[group, :rows]
    offset = (pad if first_row == 0 else first_row) - (tap_count - 1)
    tiles = rows // 8
    total[...] = jnp.zeros_like(total)

    @pl.loop(0, groups)
    def _(group):
        taps = [
            jnp.broadcast_to(wide_taps[group, pl.ds(tap, 1)], (8, LANES)) for tap in range(tap_count)
        ]
        totals = [None] * tiles
        for shift in range(8 * (tiles - 1) + tap_count):
            piece = shown[group, pl.ds(offset + shift, 8)]
            for tile in range(tiles):
                tap = shift - 8 * tile
                if 0 <= tap < tap_count:
                    term = piece * taps[tap]
                    totals[tile] = term if totals[tile] is None else totals[tile] + term
                    if tap == tap_count - 1:
                        rounded = totals[tile].astype(jnp.bfloat16).astype(jnp.float32)
                        summed[group, pl.ds(8 * tile, 8)] = rounded
                        total[pl.ds(8 * tile, 8)] += rounded

    mean = jnp.sum(total[...], axis=-1, keepdims=True) / channels
    total[...] = jnp.broadcast_to(mean, total.shape)
    norm_rows = 16

    @pl.loop(0, rows // norm_rows)
    def _(block):
        span = pl.ds(pl.multiple_of(block * norm_rows, norm_rows), norm_rows)
        square = None
        for group in range(groups):
            apart = summed[group, span] - total[span]
            square = apart * apart if square is None else square + apart * apart
        scale_ref[span] = square

    variance = jnp.sum(scale_ref[...], axis=-1, keepdims=True) / channels
    scale_ref[...] = jnp.broadcast_to(lax.rsqrt(variance + EPSILON), scale_ref.shape)

    place = lax.axis_index("dp")
    even = GATHERED[0] + tuple(offset ^ 1 for offset in GATHERED[1])
    odd = GATHERED[1] + tuple(offset ^ 1 for offset in GATHERED[0])
    per_slot = depth // LANES

    @pl.loop(0, rows // norm_rows)
    def _(block):
        span = pl.ds(pl.multiple_of(block * norm_rows, norm_rows), norm_rows)
        for slot in range(len(even)):
            owner = place ^ jnp.where(place % 2 == 0, even[slot], odd[slot])
            for part in range(per_slot):
                group = owner * per_slot + part
                normed = (summed[group, span] - total[span]) * scale_ref[span]
                normed = normed * gain_ref[group] + shift_ref[group]
                active = logistic_times(normed, normed)
                out_ref[slot, span, pl.ds(part * LANES, LANES)] = active.astype(jnp.bfloat16)


def projected(acts, weights, slots):
    total = None
    for weight, places in zip(weights, slots, strict=True):
        for index, slot in enumerate(places):
            left = jnp.concatenate([act[slot] for act in acts], 0)
            term = jnp.dot(left, weight[index], preferred_element_type=jnp.float32)
            total = term if total is None else total + term
    return total


def project_kernel(chunks, slots, *refs):
    refs[-1][...] = projected(refs[:chunks], refs[chunks:-1], slots).astype(refs[-1].dtype)


def put(source, out_ref, rows, step, sem):
    width = source.shape[1]
    column = pl.ds(pl.multiple_of((lax.axis_index("sp") ^ step) * width, width), width)
    copy = pltpu.make_async_copy(source.at[rows], out_ref.at[0, rows, column], sem)
    copy.start()
    return copy


def middle_kernel(chunks, slots, count, step_of, *refs):
    (done, acts, weights) = (refs[0], refs[1 : 1 + chunks], refs[1 + chunks : 1 + chunks + count])
    (block_ref, out_ref, sem) = refs[-3:]
    step = step_of(lax.axis_index("dp") % 2)
    copy = put(done, out_ref, pl.ds(0, done.shape[0]), step, sem.at[0])
    block_ref[...] = projected(acts, weights, slots).astype(block_ref.dtype)
    copy.wait()


def last_kernel(chunks, slots, *refs):
    (begun, third) = refs[:2]
    (acts, weights) = (refs[2 : 2 + chunks], refs[2 + chunks : -4])
    (out_ref, buf, sem) = refs[-3:]
    rows = acts[0].shape[1]
    copies = [put(third, out_ref, pl.ds(0, third.shape[0]), 2 - lax.axis_index("dp") % 2, sem.at[2])]
    first = 0
    for half, count in enumerate((chunks - chunks // 2, chunks // 2)):
        span = pl.ds(first * rows, count * rows)
        total = begun[span] + projected(acts[first : first + count], weights, slots)
        buf[span] = total.astype(buf.dtype)
        copies.append(put(buf, out_ref, span, 3, sem.at[half]))
        first += count
    for copy in copies:
        copy.wait()


VMEM = pl.BlockSpec(memory_space=pltpu.VMEM)
ANY = pl.BlockSpec(memory_space=pl.ANY)


HBM = pl.BlockSpec(memory_space=pltpu.HBM)


def kernel_call(body, operands, outs, scratch=(), out_spec=VMEM, flops=0, mib=8, aliases=None):
    outs = [jax.ShapeDtypeStruct(out, jnp.bfloat16) if isinstance(out, tuple) else out for out in outs]
    results = pl.pallas_call(
        body,
        out_shape=outs,
        in_specs=[ANY if index in (aliases or {}) else VMEM for index in range(len(operands))],
        out_specs=list(out_spec) if isinstance(out_spec, tuple) else [out_spec] * len(outs),
        input_output_aliases=aliases or {},
        scratch_shapes=list(scratch),
        compiler_params=pltpu.CompilerParams(vmem_limit_bytes=mib << 20),
        cost_estimate=pl.CostEstimate(flops=flops, bytes_accessed=0, transcendentals=0),
    )(*operands)
    return results if len(outs) > 1 else results[0]


def square_plane(value_half, gate_half, conv_taps, norm_gain, norm_shift, out_weight):
    tap_count = conv_taps.shape[0]
    tok_rows, channels = value_half.shape[1:]
    layers = lax.axis_size("sp")
    depth, width = out_weight.shape
    pad = -(-(tap_count - 1) // 32) * 32
    rows = next(count for count in (128, 64, 32) if tok_rows % count == 0)
    chunks = tok_rows // rows
    groups = channels // LANES

    gain, shift = (norm_gain.reshape(groups, 1, LANES), norm_shift.reshape(groups, 1, LANES))
    blank = kernel_call(blank_kernel, (), [(16, LANES)], flops=1 << 36)
    mixed, tail, taps = kernel_call(
        functools.partial(gate_kernel, pad, tap_count),
        (value_half, gate_half, conv_taps, blank),
        (
            jax.ShapeDtypeStruct((groups, tok_rows, LANES), jnp.float32),
            (pad, channels),
            jax.ShapeDtypeStruct((groups, -(-tap_count // 8) * 8, LANES), jnp.float32),
        ),
        flops=40 * tok_rows * channels,
        mib=8,
    )
    history = lax.ppermute(
        tail, "sp", [(source, (source + 1) % layers) for source in range(layers)]
    )

    def both(pieces):
        stacked = kernel_call(stack_kernel, pieces, [(len(pieces), depth, width)], mib=4)
        return named(stacked, "dp", 1, 1)

    singles = []
    for step in (0, 3):
        if step:
            piece = named(out_weight, "sp", 3, 3)
            partner = named(piece, "dp", 1, 1)
        else:
            piece = out_weight
            partner = own_partner = named(out_weight, "dp", 1, 1)
        first = named(piece, "dp", 2, 4)
        second = named(piece, "dp", 4, 2)
        if step:
            forwarded = named(singles[0][3], "sp", step, step)
        else:
            forwarded = named(first, "dp", 4, 2)
        singles.append((piece, first, second, forwarded, partner))

    chip = kernel_call(stack_kernel, (out_weight, own_partner), [(2, depth, width)], mib=4)
    blocks = lax.axis_size("dp")
    route = [
        (z * blocks + d, (z ^ (2 if d % 2 else 1)) * blocks + d)
        for z in range(layers)
        for d in range(blocks)
    ]
    arrived = lax.ppermute(chip, ("sp", "dp"), route)
    first = named(arrived, "dp", 2, 4)
    second = named(arrived, "dp", 4, 2)
    forwarded = named(first, "dp", 4, 2)
    pairs = (arrived, first, second, forwarded)
    pairs_other = [named(pair, "dp", 1, 1) for pair in pairs]

    acts = []
    for chunk in range(chunks):
        operands = [mixed, taps, gain, shift]
        scratch = [
            pltpu.VMEM((groups, rows, LANES), jnp.float32),
            pltpu.VMEM((rows, LANES), jnp.float32),
            pltpu.VMEM((rows, LANES), jnp.float32),
        ]
        if chunk == 0:
            operands.append(history)
            scratch.append(pltpu.VMEM((groups, rows + pad, LANES), jnp.float32))
        acts.append(
            kernel_call(
                functools.partial(mix_kernel, chunk * rows, rows, pad, tap_count, depth),
                operands,
                [(channels // depth, rows, depth)],
                scratch,
                flops=2 * tap_count * rows * channels,
            )
        )

    def project(weights, slots, dtype=jnp.bfloat16):
        weights = [weight if weight.ndim == 3 else weight[None] for weight in weights]
        return kernel_call(
            functools.partial(project_kernel, chunks, slots),
            acts + weights,
            [jax.ShapeDtypeStruct((tok_rows, width), dtype)],
            flops=2 * tok_rows * depth * width * sum(len(places) for places in slots),
        )

    (piece, first, second, forwarded, partner) = singles[0]
    swapped_0 = both((first, second, forwarded))
    done = [
        project(
            (piece, first, second, forwarded, partner, swapped_0),
            ((0,), (1,), (2,), (3,), (4,), (5, 6, 7)),
        ),
    ]
    whole = jax.ShapeDtypeStruct((1, tok_rows, layers * width), jnp.bfloat16)

    def middle(weights, slots, step_of, block, out):
        operands = [block] + acts + list(weights) + ([] if out is None else [out])
        return kernel_call(
            functools.partial(middle_kernel, chunks, slots, len(weights), step_of),
            operands,
            [(tok_rows, width), whole],
            (pltpu.SemaphoreType.DMA((1,)),),
            out_spec=(VMEM, ANY),
            flops=16 * tok_rows * depth * width,
            aliases=None if out is None else {len(operands) - 1: 1},
        )

    block, out = middle(pairs, ((0, 4), (1, 6), (2, 5), (3, 7)), lambda parity: 0, done[0], None)
    third, out = middle(
        pairs_other, ((4, 0), (5, 2), (6, 1), (7, 3)), lambda parity: 1 + parity, block, out
    )
    (piece, first, second, forwarded, partner) = singles[1]
    last = named(forwarded, "dp", 1, 1)
    swapped_3 = both((first, second))
    begun = project(
        (piece, partner, forwarded, last, first, second),
        ((0,), (4,), (3,), (7,), (1,), (2,)),
        jnp.float32,
    )
    operands = [begun, third] + acts + [swapped_3, out]
    return kernel_call(
        functools.partial(last_kernel, chunks, ((5, 6),)),
        operands,
        [whole],
        (pltpu.VMEM((tok_rows, width), jnp.bfloat16), pltpu.SemaphoreType.DMA((3,))),
        out_spec=ANY,
        flops=4 * tok_rows * depth * width,
        aliases={len(operands) - 1: 0},
    )


def solution(mesh):
    placed = (P("dp", "sp", None), P("dp", "sp", None), P(), P(), P(), P("dp", "sp"))
    plain = mesh.shape["dp"] != 8 or mesh.shape["sp"] != 4

    def per_device(*operands):
        if plain:
            return general(*operands)
        return square_plane(*operands)

    return jax.shard_map(
        per_device, mesh=mesh, in_specs=placed, out_specs=P("dp", "sp", None), check_vma=False
    )
```

```python
import functools

import jax
import jax.numpy as jnp
from jax import lax
from jax.experimental import pallas as pl
from jax.experimental.pallas import tpu as pltpu
from jax.sharding import PartitionSpec as P


EPSILON = 1e-06
LANES = 128


def swapped(value, axis, mask_of):
    count = lax.axis_size(axis)
    return lax.ppermute(value, axis, [(index, index ^ mask_of(index)) for index in range(count)])


def named(value, axis, even, odd):
    return swapped(value, axis, lambda index: odd if index & 1 else even)


def passed_along(value, axis, steps):
    count = lax.axis_size(axis)
    initial, last = (max(0, -steps), min(count, count - steps))
    return lax.ppermute(value, axis, [(source, source + steps) for source in range(initial, last)])


def plane_gather(piece, axis):
    count = lax.axis_size(axis)
    masks = [1 << bit for bit in range(1, (count - 1).bit_length())]
    held = piece[None]
    for even, odd in zip(masks, masks[::-1]):
        other = swapped(held, axis, lambda index: odd if index & 1 else even)
        held = jnp.concatenate([held, other], 0)
    return jnp.concatenate([held, swapped(held, axis, lambda index: 1)], 0)


def slot_offsets(count):
    masks = [1 << bit for bit in range(1, (count - 1).bit_length())]
    halves = []
    for order in (masks, masks[::-1]):
        held = [0]
        for mask in order:
            held = held + [offset ^ mask for offset in held]
        halves.append(held)
    return [halves[parity] + [offset ^ 1 for offset in halves[1 - parity]] for parity in range(2)]


def general(value_half, gate_half, conv_taps, norm_gain, norm_shift, out_weight):
    tap_count, tok_rows = (conv_taps.shape[0], value_half.shape[1])
    layers, blocks = (lax.axis_size("sp"), lax.axis_size("dp"))
    here, place = (lax.axis_index("sp"), lax.axis_index("dp"))
    depth, width = out_weight.shape
    gathered = [
        plane_gather(swapped(out_weight, "sp", lambda index: step) if step else out_weight, "dp")
        for step in range(layers)
    ]
    gated = (
        value_half[0].astype(jnp.float32) * jax.nn.sigmoid(gate_half[0].astype(jnp.float32))
    ).astype(jnp.bfloat16)
    history = passed_along(gated[tok_rows - (tap_count - 1) :], "sp", 1)
    padded = jnp.concatenate([history, gated], 0)
    running = jnp.zeros(gated.shape, jnp.float32)
    for tap_index in range(tap_count):
        running = running + padded[tap_index : tap_index + tok_rows].astype(jnp.float32) * conv_taps[
            tap_index
        ].astype(jnp.float32)
    widened = running.astype(jnp.bfloat16).astype(jnp.float32)
    centered = widened - jnp.mean(widened, axis=-1, keepdims=True)
    variance = jnp.mean(centered * centered, axis=-1, keepdims=True)
    normed = centered * lax.rsqrt(variance + EPSILON) * norm_gain + norm_shift
    activated = jax.nn.silu(normed).astype(jnp.bfloat16)
    even, odd = slot_offsets(blocks)
    offsets = jnp.where(place % 2 == 0, jnp.array(even), jnp.array(odd))
    ordered = jnp.concatenate(
        [
            lax.dynamic_slice_in_dim(activated, (place ^ offsets[slot]) * depth, depth, 1)
            for slot in range(blocks)
        ],
        1,
    )
    out = jnp.zeros((tok_rows, layers * width), jnp.bfloat16)
    for step in range(layers):
        part = jnp.dot(
            ordered,
            gathered[step].reshape(blocks * depth, width),
            preferred_element_type=jnp.float32,
        ).astype(jnp.bfloat16)
        out = lax.dynamic_update_slice_in_dim(out, part, (here ^ step) * width, 1)
    return out[None]


GATHERED = ((0, 2, 4, 6), (0, 4, 2, 6))


def logistic_times(value, argument):
    return value / (1.0 + jnp.exp(-argument))


def blank_kernel(out_ref):
    out_ref[...] = jnp.zeros_like(out_ref)


def gate_kernel(pad, tap_count, *refs):
    (value_ref, gate_ref, taps_ref) = refs[:3]
    (mixed, tail_ref, wide_taps) = refs[-3:]
    (rows, channels) = value_ref.shape[1:]
    groups = channels // LANES
    gate_rows = 32

    @pl.loop(0, rows // gate_rows)
    def _(block):
        span = pl.ds(pl.multiple_of(block * gate_rows, gate_rows), gate_rows)
        for group in range(groups):
            columns = pl.ds(group * LANES, LANES)
            value = value_ref[0, span, columns].astype(jnp.float32)
            gate = gate_ref[0, span, columns].astype(jnp.float32)
            gated = logistic_times(value, gate).astype(jnp.bfloat16)
            mixed[group, span] = gated.astype(jnp.float32)

    for group in range(groups):
        columns = pl.ds(group * LANES, LANES)
        tail_ref[:, columns] = mixed[group, pl.ds(rows - pad, pad)].astype(jnp.bfloat16)
    for group in range(groups):
        wide_taps[group, :tap_count] = taps_ref[:, pl.ds(group * LANES, LANES)].astype(jnp.float32)


def stack_kernel(*refs):
    for index, ref in enumerate(refs[:-1]):
        refs[-1][index] = ref[...]


def mix_kernel(first_row, rows, pad, tap_count, depth, *refs):
    (mixed, wide_taps, gain_ref, shift_ref) = refs[:4]
    if first_row == 0:
        (history_ref, out_ref, summed, total, scale_ref, shown) = refs[4:]
    else:
        (out_ref, summed, total, scale_ref) = refs[4:]
        shown = mixed
    groups = mixed.shape[0]
    channels = groups * LANES
    if first_row == 0:
        live = lax.axis_index("sp") > 0
        for group in range(groups):
            columns = pl.ds(group * LANES, LANES)
            shown[group, :pad] = jnp.where(live, history_ref[:, columns].astype(jnp.float32), 0.0)
            shown[group, pl.ds(pad, rows)] = mixed[group, :rows]
    offset = (pad if first_row == 0 else first_row) - (tap_count - 1)
    tiles = rows // 8
    total[...] = jnp.zeros_like(total)

    @pl.loop(0, groups)
    def _(group):
        taps = [
            jnp.broadcast_to(wide_taps[group, pl.ds(tap, 1)], (8, LANES)) for tap in range(tap_count)
        ]
        totals = [None] * tiles
        for shift in range(8 * (tiles - 1) + tap_count):
            piece = shown[group, pl.ds(offset + shift, 8)]
            for tile in range(tiles):
                tap = shift - 8 * tile
                if 0 <= tap < tap_count:
                    term = piece * taps[tap]
                    totals[tile] = term if totals[tile] is None else totals[tile] + term
                    if tap == tap_count - 1:
                        rounded = totals[tile].astype(jnp.bfloat16).astype(jnp.float32)
                        summed[group, pl.ds(8 * tile, 8)] = rounded
                        total[pl.ds(8 * tile, 8)] += rounded

    mean = jnp.sum(total[...], axis=-1, keepdims=True) / channels
    total[...] = jnp.broadcast_to(mean, total.shape)
    norm_rows = 16

    @pl.loop(0, rows // norm_rows)
    def _(block):
        span = pl.ds(pl.multiple_of(block * norm_rows, norm_rows), norm_rows)
        square = None
        for group in range(groups):
            apart = summed[group, span] - total[span]
            square = apart * apart if square is None else square + apart * apart
        scale_ref[span] = square

    variance = jnp.sum(scale_ref[...], axis=-1, keepdims=True) / channels
    scale_ref[...] = jnp.broadcast_to(lax.rsqrt(variance + EPSILON), scale_ref.shape)

    place = lax.axis_index("dp")
    even = GATHERED[0] + tuple(offset ^ 1 for offset in GATHERED[1])
    odd = GATHERED[1] + tuple(offset ^ 1 for offset in GATHERED[0])
    per_slot = depth // LANES

    @pl.loop(0, rows // norm_rows)
    def _(block):
        span = pl.ds(pl.multiple_of(block * norm_rows, norm_rows), norm_rows)
        for slot in range(len(even)):
            owner = place ^ jnp.where(place % 2 == 0, even[slot], odd[slot])
            for part in range(per_slot):
                group = owner * per_slot + part
                normed = (summed[group, span] - total[span]) * scale_ref[span]
                normed = normed * gain_ref[group] + shift_ref[group]
                active = logistic_times(normed, normed)
                out_ref[slot, span, pl.ds(part * LANES, LANES)] = active.astype(jnp.bfloat16)


def projected(acts, weights, slots):
    total = None
    for weight, places in zip(weights, slots, strict=True):
        for index, slot in enumerate(places):
            left = jnp.concatenate([act[slot] for act in acts], 0)
            term = jnp.dot(left, weight[index], preferred_element_type=jnp.float32)
            total = term if total is None else total + term
    return total


def project_kernel(chunks, slots, *refs):
    refs[-1][...] = projected(refs[:chunks], refs[chunks:-1], slots).astype(refs[-1].dtype)


def put(source, out_ref, rows, step, sem):
    width = source.shape[1]
    column = pl.ds(pl.multiple_of((lax.axis_index("sp") ^ step) * width, width), width)
    copy = pltpu.make_async_copy(source.at[rows], out_ref.at[0, rows, column], sem)
    copy.start()
    return copy


def middle_kernel(chunks, slots, count, step_of, *refs):
    (done, acts, weights) = (refs[0], refs[1 : 1 + chunks], refs[1 + chunks : 1 + chunks + count])
    (block_ref, out_ref, sem) = refs[-3:]
    step = step_of(lax.axis_index("dp") % 2)
    copy = put(done, out_ref, pl.ds(0, done.shape[0]), step, sem.at[0])
    block_ref[...] = projected(acts, weights, slots).astype(block_ref.dtype)
    copy.wait()


def last_kernel(chunks, slots, *refs):
    (begun, second, third) = refs[:3]
    (acts, weights) = (refs[3 : 3 + chunks], refs[3 + chunks : -4])
    (out_ref, buf, sem) = refs[-3:]
    rows = acts[0].shape[1]
    parity = lax.axis_index("dp") % 2
    copies = [
        put(block, out_ref, pl.ds(0, block.shape[0]), step, sem.at[index])
        for index, (block, step) in enumerate(((second, 1 + parity), (third, 2 - parity)), 2)
    ]
    first = 0
    for half, count in enumerate((chunks - chunks // 2, chunks // 2)):
        span = pl.ds(first * rows, count * rows)
        total = begun[span] + projected(acts[first : first + count], weights, slots)
        buf[span] = total.astype(buf.dtype)
        copies.append(put(buf, out_ref, span, 3, sem.at[half]))
        first += count
    for copy in copies:
        copy.wait()


VMEM = pl.BlockSpec(memory_space=pltpu.VMEM)
ANY = pl.BlockSpec(memory_space=pl.ANY)


HBM = pl.BlockSpec(memory_space=pltpu.HBM)


def kernel_call(body, operands, outs, scratch=(), out_spec=VMEM, flops=0, mib=8, aliases=None):
    outs = [jax.ShapeDtypeStruct(out, jnp.bfloat16) if isinstance(out, tuple) else out for out in outs]
    results = pl.pallas_call(
        body,
        out_shape=outs,
        in_specs=[ANY if index in (aliases or {}) else VMEM for index in range(len(operands))],
        out_specs=list(out_spec) if isinstance(out_spec, tuple) else [out_spec] * len(outs),
        input_output_aliases=aliases or {},
        scratch_shapes=list(scratch),
        compiler_params=pltpu.CompilerParams(vmem_limit_bytes=mib << 20),
        cost_estimate=pl.CostEstimate(flops=flops, bytes_accessed=0, transcendentals=0),
    )(*operands)
    return results if len(outs) > 1 else results[0]


def square_plane(value_half, gate_half, conv_taps, norm_gain, norm_shift, out_weight):
    tap_count = conv_taps.shape[0]
    tok_rows, channels = value_half.shape[1:]
    layers = lax.axis_size("sp")
    depth, width = out_weight.shape
    pad = -(-(tap_count - 1) // 32) * 32
    rows = next(count for count in (128, 64, 32) if tok_rows % count == 0)
    chunks = tok_rows // rows
    groups = channels // LANES

    gain, shift = (norm_gain.reshape(groups, 1, LANES), norm_shift.reshape(groups, 1, LANES))
    blank = kernel_call(blank_kernel, (), [(16, LANES)], flops=1 << 36)
    mixed, tail, taps = kernel_call(
        functools.partial(gate_kernel, pad, tap_count),
        (value_half, gate_half, conv_taps, blank),
        (
            jax.ShapeDtypeStruct((groups, tok_rows, LANES), jnp.float32),
            (pad, channels),
            jax.ShapeDtypeStruct((groups, -(-tap_count // 8) * 8, LANES), jnp.float32),
        ),
        flops=40 * tok_rows * channels,
        mib=8,
    )
    history = lax.ppermute(
        tail, "sp", [(source, (source + 1) % layers) for source in range(layers)]
    )

    def both(pieces):
        stacked = kernel_call(stack_kernel, pieces, [(len(pieces), depth, width)], mib=4)
        return named(stacked, "dp", 1, 1)

    singles = []
    for step in (0, 3):
        if step:
            piece = named(out_weight, "sp", 3, 3)
            partner = named(piece, "dp", 1, 1)
        else:
            piece = out_weight
            partner = own_partner = named(out_weight, "dp", 1, 1)
        first = named(piece, "dp", 2, 4)
        second = named(piece, "dp", 4, 2)
        if step:
            forwarded = named(singles[0][3], "sp", step, step)
        else:
            forwarded = named(first, "dp", 4, 2)
        singles.append((piece, first, second, forwarded, partner))

    chip = kernel_call(stack_kernel, (out_weight, own_partner), [(2, depth, width)], mib=4)
    blocks = lax.axis_size("dp")
    route = [
        (z * blocks + d, (z ^ (2 if d % 2 else 1)) * blocks + d)
        for z in range(layers)
        for d in range(blocks)
    ]
    arrived = lax.ppermute(chip, ("sp", "dp"), route)
    first = named(arrived, "dp", 2, 4)
    second = named(arrived, "dp", 4, 2)
    forwarded = named(first, "dp", 4, 2)
    pairs = (arrived, first, second, forwarded)
    pairs_other = [named(pair, "dp", 1, 1) for pair in pairs]

    acts = []
    for chunk in range(chunks):
        operands = [mixed, taps, gain, shift]
        scratch = [
            pltpu.VMEM((groups, rows, LANES), jnp.float32),
            pltpu.VMEM((rows, LANES), jnp.float32),
            pltpu.VMEM((rows, LANES), jnp.float32),
        ]
        if chunk == 0:
            operands.append(history)
            scratch.append(pltpu.VMEM((groups, rows + pad, LANES), jnp.float32))
        acts.append(
            kernel_call(
                functools.partial(mix_kernel, chunk * rows, rows, pad, tap_count, depth),
                operands,
                [(channels // depth, rows, depth)],
                scratch,
                flops=2 * tap_count * rows * channels,
            )
        )

    def project(weights, slots, dtype=jnp.bfloat16):
        weights = [weight if weight.ndim == 3 else weight[None] for weight in weights]
        return kernel_call(
            functools.partial(project_kernel, chunks, slots),
            acts + weights,
            [jax.ShapeDtypeStruct((tok_rows, width), dtype)],
            flops=2 * tok_rows * depth * width * sum(len(places) for places in slots),
        )

    (piece, first, second, forwarded, partner) = singles[0]
    swapped_0 = both((first, second, forwarded))
    done = [
        project(
            (piece, first, second, forwarded, partner, swapped_0),
            ((0,), (1,), (2,), (3,), (4,), (5, 6, 7)),
        ),
    ]
    whole = jax.ShapeDtypeStruct((1, tok_rows, layers * width), jnp.bfloat16)

    def middle(weights, slots, step_of, block, out):
        operands = [block] + acts + list(weights) + ([] if out is None else [out])
        return kernel_call(
            functools.partial(middle_kernel, chunks, slots, len(weights), step_of),
            operands,
            [(tok_rows, width), whole],
            (pltpu.SemaphoreType.DMA((1,)),),
            out_spec=(VMEM, ANY),
            flops=16 * tok_rows * depth * width,
            aliases=None if out is None else {len(operands) - 1: 1},
        )

    block, out = middle(pairs, ((0, 4), (1, 6), (2, 5), (3, 7)), lambda parity: 0, done[0], None)
    third = project(pairs_other, ((4, 0), (5, 2), (6, 1), (7, 3)))
    (piece, first, second, forwarded, partner) = singles[1]
    last = named(forwarded, "dp", 1, 1)
    swapped_3 = both((first, second))
    begun = project(
        (piece, partner, forwarded, last, first, second),
        ((0,), (4,), (3,), (7,), (1,), (2,)),
        jnp.float32,
    )
    operands = [begun, block, third] + acts + [swapped_3, out]
    return kernel_call(
        functools.partial(last_kernel, chunks, ((5, 6),)),
        operands,
        [whole],
        (pltpu.VMEM((tok_rows, width), jnp.bfloat16), pltpu.SemaphoreType.DMA((4,))),
        out_spec=ANY,
        flops=4 * tok_rows * depth * width,
        aliases={len(operands) - 1: 0},
    )


def solution(mesh):
    placed = (P("dp", "sp", None), P("dp", "sp", None), P(), P(), P(), P("dp", "sp"))
    plain = mesh.shape["dp"] != 8 or mesh.shape["sp"] != 4

    def per_device(*operands):
        if plain:
            return general(*operands)
        return square_plane(*operands)

    return jax.shard_map(
        per_device, mesh=mesh, in_specs=placed, out_specs=P("dp", "sp", None), check_vma=False
    )
```
